32 devices in a mesh: sp: 16 (over z, y, x), tp: 2 (over core).
Axes of the slice: x: 2, y: 2, z: 4, core: 2. Of those that a mesh axis runs over, the one named last changes fastest.
Arguments:
- residual: bfloat16 [4096, 2048], P(('sp', 'tp')), may hold values from -6 to 6
- queries: bfloat16 [4096, 1152], P('sp', 'tp'), may hold values from -800 to 800
- latent: bfloat16 [4096, 256], P('sp'), may hold values from -6 to 6
- rope_key: bfloat16 [4096, 32], P('sp'), may hold values from -6 to 6
- doc_ids: int32 [4096], P('sp'), may hold values from 0 to 5, never falling along the last dimension, each value on 1 to 2048 neighbouring positions
- latent_to_key: bfloat16 [256, 768], P(None, 'tp'), may hold values from -0.375 to 0.375
- latent_to_value: bfloat16 [256, 768], P(None, 'tp'), may hold values from -0.375 to 0.375
- out_proj: bfloat16 [768, 2048], replicated, may hold values from -0.21875 to 0.21875
- mix_gain: float32 [2048], replicated, may hold values from 0.1 to 1.9
- moe_gain: float32 [2048], replicated, may hold values from 0.1 to 1.9
- expert_ids: int32 [4096, 2], P(('sp', 'tp')), may hold values from 0 to 15, as said below
- route_weight: float32 [4096, 2], P(('sp', 'tp')), may hold values from 0.1 to 1
- gate_weight: bfloat16 [16, 2048, 1024], P('sp', None, 'tp'), may hold values from -0.125 to 0.125
- up_weight: bfloat16 [16, 2048, 1024], P('sp', None, 'tp'), may hold values from -0.125 to 0.125
- down_weight: bfloat16 [16, 1024, 2048], P('sp', 'tp'), may hold values from -0.1875 to 0.1875
Outputs:
- output: bfloat16 [4096, 2048], P(('sp', 'tp'))
The draws below stay inside these ranges and needn't reach their ends.
Inputs may be any that keep to these rules, and one draw needn't show every extreme that they name: `expert_ids`: each row names 2 different experts of one group of 4 consecutive numbers; in each aligned block of 128 rows (the rows of one device) no expert is named more than 32 times, and some expert exactly 32 times.
All inputs are finite; a program needn't handle non-finite values.
Results may differ from the reference program's by a relative error of at most 0.013.
Values may be sent and summed in bfloat16 or wider, within the bound.
A program may use at most 64 MiB of HBM per device.

```python
import math
import jax
import jax.numpy as jnp
import numpy as np
from jax import lax

D = 2048
HEAD_COUNT = 12
UNROTATED_DIM = 64
ROPE = 32
VALUE_ENTRIES = 64
LATENT_RANK = 256
FF = 1024
GROUPS = 4
TOP_K = 2
TOK_DEV = 256
TOKEN_COUNT = 4096
EXPERTS = 16
N_TP = 2


def rope_rows(key):
    drawn = jax.random.normal(jax.random.fold_in(key, 11), (TOKEN_COUNT, ROPE), jnp.float32)
    return jnp.clip(drawn, -6.0, 6.0)


def draw_rope_key(key, part):
    return rope_rows(key).astype(jnp.bfloat16)


def draw_queries(key, part):
    normal_part = jax.random.normal(jax.random.fold_in(key, 12), (TOKEN_COUNT, HEAD_COUNT, UNROTATED_DIM + ROPE), jnp.float32)
    normal_part = jnp.clip(normal_part, -6.0, 6.0)
    return normal_part.reshape(TOKEN_COUNT, HEAD_COUNT * (UNROTATED_DIM + ROPE)).astype(jnp.bfloat16)


def draw_expert_ids(key, part):
    row_count = TOK_DEV // N_TP
    half_rows = row_count // 2
    block_count = TOKEN_COUNT // row_count
    per_group = EXPERTS // GROUPS
    full_group = jax.random.randint(jax.random.fold_in(key, 1), (), 0, GROUPS)
    others = jax.random.randint(jax.random.fold_in(key, 2), (block_count, half_rows), 0, GROUPS - 1)
    others = others + (others >= full_group).astype(jnp.int32)
    group_ids = jnp.concatenate([jnp.full((block_count, half_rows), full_group, jnp.int32), others], axis=1)
    block_keys = jax.random.split(jax.random.fold_in(key, 3), block_count)
    group_ids = jax.vmap(lambda block_key, row_groups: jax.random.permutation(block_key, row_groups))(block_keys, group_ids)
    onehot = (group_ids[..., None] == jnp.arange(GROUPS, dtype=jnp.int32)).astype(jnp.int32)
    earlier = jnp.cumsum(onehot, axis=1) - onehot
    slot_rank = jnp.sum(earlier * onehot, axis=-1)
    offsets = jax.random.randint(jax.random.fold_in(key, 4), (block_count, GROUPS), 0, per_group)
    spacing = jax.random.randint(jax.random.fold_in(key, 5), (block_count, GROUPS), 1, per_group)
    own_offset = jnp.take_along_axis(offsets, group_ids, axis=1)
    own_spacing = jnp.take_along_axis(spacing, group_ids, axis=1)
    first_pick = (slot_rank + own_offset) % per_group
    second_pick = (slot_rank + own_offset + own_spacing) % per_group
    chosen = jnp.stack([group_ids * per_group + first_pick, group_ids * per_group + second_pick], axis=-1)
    return chosen.reshape(TOKEN_COUNT, 2).astype(jnp.int32)


def steps_of(own_key, shape, cuts, least, top_value):
    level, own = 1.0, jax.random.fold_in(own_key, 6)
    for axis_at, blocks in cuts:
        draws = jnp.exp(jax.random.uniform(jax.random.fold_in(own, axis_at), (blocks,), jnp.float32, least / len(cuts), top_value / len(cuts)))
        level = level * jnp.repeat(draws, shape[axis_at] // blocks).reshape([-1 if axis == axis_at else 1 for axis in range(len(shape))])
    return level


def profile(number_of, total, bound, slope):
    weights = [(1 << 20) // math.isqrt(rank ** slope) + 1 for rank in range(2, number_of + 1)]
    spare, counts = total - bound - (number_of - 1), [1] * (number_of - 1)
    while spare > 0:
        free = [i for i in range(number_of - 1) if counts[i] < bound]
        mass, remaining = sum([weights[i] for i in free]), spare
        for i in free:
            extra = min(bound - counts[i], max(1, remaining * weights[i] // mass), spare)
            counts[i] = counts[i] + extra
            spare = spare - extra
    return np.array([bound] + counts)


def uneven_parts(own_key, amount, total, limit, slope):
    if amount == 2:
        one = jax.random.randint(own_key, (), max(1, total - limit), min(limit, total - 1) + 1)
        return jnp.stack([one, total - one])
    tallies = jnp.asarray(profile(amount, total, limit, slope), jnp.int32)
    twos = (amount - 1) // 2
    source_of, sink = tallies[1:1 + 2 * twos:2], tallies[2:2 + 2 * twos:2]
    room = jnp.minimum(source_of - 1, limit - sink)
    moved = jax.random.randint(jax.random.fold_in(own_key, 1), (twos,), 0, 1 << 20) % (room + 1)
    tallies = tallies.at[1:1 + 2 * twos:2].set(source_of - moved).at[2:2 + 2 * twos:2].set(sink + moved)
    return tallies[jax.random.permutation(jax.random.fold_in(own_key, 2), amount)]


def bell_draw(key, extent, scale, most, cuts=(), held_as=jnp.bfloat16):
    values = scale * jax.random.normal(key, extent, jnp.float32)
    if cuts:
        values = values * steps_of(key, extent, cuts, -0.22, 0.18)
    return jnp.clip(values, -most, most).astype(held_as)


def setup_inputs(seed: int = 0) -> dict:
    arg_keys = jax.random.split(jax.random.key(seed), 16)
    return {
        "residual": bell_draw(arg_keys[0], (TOKEN_COUNT, D), 1.0, 6.0, ((0, 32),)),
        "queries": draw_queries(jax.random.fold_in(arg_keys[15], 71), 0),
        "latent": bell_draw(arg_keys[2], (TOKEN_COUNT, LATENT_RANK), 1.0, 6.0, ((0, 16),)),
        "rope_key": draw_rope_key(jax.random.fold_in(arg_keys[15], 71), 0),
        "doc_ids": jnp.searchsorted(jnp.cumsum(uneven_parts(arg_keys[4], 6, TOKEN_COUNT, TOKEN_COUNT // 2, 0)), jnp.arange(TOKEN_COUNT), side="right").astype(jnp.int32),
        "latent_to_key": bell_draw(arg_keys[5], (LATENT_RANK, HEAD_COUNT * UNROTATED_DIM), LATENT_RANK ** -0.5, 0.375, ((1, 2),)),
        "latent_to_value": bell_draw(arg_keys[6], (LATENT_RANK, HEAD_COUNT * VALUE_ENTRIES), LATENT_RANK ** -0.5, 0.375, ((1, 2),)),
        "out_proj": bell_draw(arg_keys[7], (HEAD_COUNT * VALUE_ENTRIES, D), (HEAD_COUNT * VALUE_ENTRIES) ** -0.5, 0.21875),
        "mix_gain": jnp.clip(1.0 + 0.18 * jax.random.normal(arg_keys[8], (D,), jnp.float32), 0.1, 1.9),
        "moe_gain": jnp.clip(1.0 + 0.18 * jax.random.normal(arg_keys[9], (D,), jnp.float32), 0.1, 1.9),
        "expert_ids": draw_expert_ids(jax.random.fold_in(arg_keys[15], 71), 0),
        "route_weight": jnp.clip(0.1 + 0.9 * jax.random.uniform(arg_keys[11], (TOKEN_COUNT, TOP_K), jnp.float32) ** steps_of(arg_keys[11], (TOKEN_COUNT, TOP_K), ((0, 32),), -0.2, 0.2), 0.1, 1.0),
        "gate_weight": bell_draw(arg_keys[12], (EXPERTS, D, FF), D ** -0.5, 0.125, ((0, 16), (2, 2))),
        "up_weight": bell_draw(arg_keys[13], (EXPERTS, D, FF), D ** -0.5, 0.125, ((0, 16), (2, 2))),
        "down_weight": bell_draw(arg_keys[14], (EXPERTS, FF, D), FF ** -0.5, 0.1875, ((0, 16), (1, 2))),
    }


rope_base = 10000.0
epsilon = 1e-06
query_rows = 256

def rotate(source, positions):
    half_width = source.shape[-1] // 2
    frequency = rope_base ** (-jnp.arange(half_width, dtype=jnp.float32) / half_width)
    angles = positions.astype(jnp.float32)[:, None] * frequency[None, :]
    if source.ndim == 3:
        angles = angles[:, None, :]
    cosine = jnp.cos(angles)
    sine_part = jnp.sin(angles)
    upper_half = source[..., :half_width].astype(jnp.float32)
    lower_half = source[..., half_width:].astype(jnp.float32)
    turned = jnp.concatenate([upper_half * cosine - lower_half * sine_part, lower_half * cosine + upper_half * sine_part], axis=-1)
    return turned.astype(jnp.bfloat16)

def rms_scale(source, gain):
    return source * lax.rsqrt(lax.optimization_barrier(jnp.mean(source * source, axis=-1, keepdims=True)) + epsilon) * gain

def reference(residual, queries, latent, rope_key, doc_ids, latent_to_key, latent_to_value, out_proj, mix_gain, moe_gain, expert_ids, route_weight, gate_weight, up_weight, down_weight):
    positions = jnp.arange(TOKEN_COUNT, dtype=jnp.int32)
    key_nope = jnp.dot(latent, latent_to_key, preferred_element_type=jnp.float32).astype(jnp.bfloat16)
    key_nope = key_nope.reshape(TOKEN_COUNT, HEAD_COUNT, UNROTATED_DIM).astype(jnp.float32)
    values = jnp.dot(latent, latent_to_value, preferred_element_type=jnp.float32).astype(jnp.bfloat16)
    values = values.reshape(TOKEN_COUNT, HEAD_COUNT, VALUE_ENTRIES).astype(jnp.float32)
    key_rot = rotate(rope_key, positions).astype(jnp.float32)
    shaped = queries.reshape(TOKEN_COUNT, HEAD_COUNT, UNROTATED_DIM + ROPE)
    query_nope = shaped[..., :UNROTATED_DIM]
    query_rot = rotate(shaped[..., UNROTATED_DIM:], positions)
    score_scale = (UNROTATED_DIM + ROPE) ** (-0.5)
    block_count = TOKEN_COUNT // query_rows

    def attend_rows(bundle):
        nope_block, rot_block, pos_block, doc_block = bundle
        scores = (jnp.einsum('qhd,khd->qhk', nope_block.astype(jnp.float32), key_nope) + jnp.einsum('qhr,kr->qhk', rot_block.astype(jnp.float32), key_rot)) * score_scale
        allowed = ((positions[None, :] <= pos_block[:, None]) & (doc_ids[None, :] == doc_block[:, None]))[:, None, :]
        row_max = lax.optimization_barrier(jnp.max(jnp.where(allowed, scores, -jnp.inf), axis=-1, keepdims=True))
        weights = jnp.where(allowed, jnp.exp(scores - row_max), 0.0)
        totals = lax.optimization_barrier(jnp.sum(weights, axis=-1))
        rounded = lax.optimization_barrier(weights.astype(jnp.bfloat16)).astype(jnp.float32)
        mixed = jnp.einsum('qhk,khd->qhd', rounded, values) / totals[..., None]
        return mixed.astype(jnp.bfloat16).reshape(query_rows, HEAD_COUNT * VALUE_ENTRIES)
    attended = lax.map(attend_rows, (query_nope.reshape(block_count, query_rows, HEAD_COUNT, UNROTATED_DIM), query_rot.reshape(block_count, query_rows, HEAD_COUNT, ROPE), positions.reshape(block_count, query_rows), doc_ids.reshape(block_count, query_rows)))
    attended = attended.reshape(TOKEN_COUNT, HEAD_COUNT * VALUE_ENTRIES)
    mix = jnp.dot(attended, out_proj, preferred_element_type=jnp.float32)
    branch = rms_scale(mix, mix_gain)
    middle = lax.optimization_barrier((residual.astype(jnp.float32) + branch).astype(jnp.bfloat16))
    normed = rms_scale(middle.astype(jnp.float32), moe_gain).astype(jnp.bfloat16)
    row_count = TOK_DEV // N_TP
    groups_blocks = TOKEN_COUNT // row_count
    per_group = EXPERTS // GROUPS
    capacity = row_count // per_group
    flat_ids = expert_ids.reshape(groups_blocks, row_count * TOP_K)
    onehot = (flat_ids[..., None] == jnp.arange(EXPERTS, dtype=jnp.int32)).astype(jnp.int32)
    earlier = jnp.cumsum(onehot, axis=1) - onehot
    slot_rank = lax.optimization_barrier(jnp.sum(earlier * onehot, axis=-1)).astype(jnp.int32)
    block_index = jnp.broadcast_to(jnp.arange(groups_blocks, dtype=jnp.int32)[:, None], flat_ids.shape)
    token_index = (block_index * row_count + jnp.arange(row_count * TOP_K, dtype=jnp.int32)[None, :] // TOP_K).astype(jnp.int32)
    row_table = jnp.full((EXPERTS, groups_blocks, capacity), TOKEN_COUNT, jnp.int32)
    row_table = row_table.at[flat_ids, block_index, slot_rank].set(token_index)
    weight_table = jnp.zeros((EXPERTS, groups_blocks, capacity), jnp.float32)
    weight_table = weight_table.at[flat_ids, block_index, slot_rank].set(route_weight.reshape(groups_blocks, row_count * TOP_K))
    padded = jnp.concatenate([normed, jnp.zeros((1, D), jnp.bfloat16)], axis=0)
    half_units = FF // N_TP

    def expert_step(accumulated, inputs):
        table_rows, table_weights, gate_mat, up_mat, down_mat = inputs
        picked = padded[table_rows.reshape(-1)]
        gate_out = jnp.dot(picked, gate_mat, preferred_element_type=jnp.float32)
        up_out = jnp.dot(picked, up_mat, preferred_element_type=jnp.float32)
        hidden = (jax.nn.silu(gate_out) * up_out).astype(jnp.bfloat16)
        combined = jnp.zeros((picked.shape[0], D), jnp.float32)
        for portion in range(N_TP):
            partial_value = jnp.dot(hidden[:, portion * half_units:(portion + 1) * half_units], down_mat[portion * half_units:(portion + 1) * half_units], preferred_element_type=jnp.float32)
            combined = combined + lax.optimization_barrier(partial_value.astype(jnp.bfloat16)).astype(jnp.float32)
        result = lax.optimization_barrier(combined.astype(jnp.bfloat16)).astype(jnp.float32)
        accumulated = accumulated.at[table_rows.reshape(-1)].add(result * table_weights.reshape(-1)[:, None])
        return (accumulated, None)
    accumulated, _ = lax.scan(expert_step, jnp.zeros((TOKEN_COUNT + 1, D), jnp.float32), (row_table, weight_table, gate_weight, up_weight, down_weight))
    return (middle.astype(jnp.float32) + accumulated[:TOKEN_COUNT]).astype(jnp.bfloat16)
```

```python
import functools
import math

import jax
import jax.numpy as jnp
from jax import lax
from jax.experimental import pallas as pl
from jax.experimental.pallas import tpu as pltpu
from jax.sharding import PartitionSpec as P

UNROTATED_DIM = 64
ROPE = 32
VALUE_ENTRIES = 64
GROUPS = 4
HEAD_LANES = 128

rope_base = 10000.0
epsilon = 1e-06


def angles_of(positions):
    half_width = ROPE // 2
    frequency = rope_base ** (-jnp.arange(half_width, dtype=jnp.float32) / half_width)
    angles = positions.astype(jnp.float32)[:, None] * frequency[None, :]
    return jnp.cos(angles), jnp.sin(angles)


def rms_scale(source, gain):
    return source * lax.rsqrt(jnp.mean(source * source, axis=-1, keepdims=True) + epsilon) * gain


def attention_kernel(
    heads, block, lo_ref, query_ref, table_ref, span_ref, packed_ref, wk_ref, wv_ref, out_ref,
    turned, high, total, acc,
):
    rows = query_ref.shape[0]
    width = query_ref.shape[1]
    rank = wk_ref.shape[0]
    per_head = UNROTATED_DIM + ROPE
    cosine = table_ref[:, :HEAD_LANES]
    sine = table_ref[:, HEAD_LANES:]
    for h in range(heads):
        first = h * per_head // 128 * 128
        last = min(-(-(h + 1) * per_head // 128) * 128, width)
        window = query_ref[:, first:last]
        shape = (last - first, HEAD_LANES)
        source = lax.broadcasted_iota(jnp.int32, shape, 0) + (first - h * per_head)
        lane = lax.broadcasted_iota(jnp.int32, shape, 1)
        half = ROPE // 2
        plain = jnp.where((source == lane) & (lane < per_head), 1.0, 0.0).astype(jnp.bfloat16)
        upper = (lane >= UNROTATED_DIM) & (lane < UNROTATED_DIM + half) & (source == lane + half)
        lower = (lane >= UNROTATED_DIM + half) & (lane < per_head) & (source == lane - half)
        crossed = (jnp.where(lower, 1.0, 0.0) - jnp.where(upper, 1.0, 0.0)).astype(jnp.bfloat16)
        straight = jnp.dot(window, plain, preferred_element_type=jnp.float32)
        swapped = jnp.dot(window, crossed, preferred_element_type=jnp.float32)
        turned[h] = (straight * cosine + swapped * sine).astype(jnp.bfloat16)
    high[...] = jnp.full(high.shape, -1e30, jnp.float32)
    total[...] = jnp.zeros(total.shape, jnp.float32)
    acc[...] = jnp.zeros(acc.shape, jnp.float32)
    span_first = span_ref[0:1, :]
    span_last = span_ref[1:2, :]
    scale = per_head ** (-0.5)

    def step(number, carry):
        base = pl.multiple_of(number * block, block)
        latent = packed_ref[pl.ds(base, block), :rank]
        extra = packed_ref[pl.ds(base, block), rank:]
        position = base + lax.broadcasted_iota(jnp.int32, (block, rows), 0)
        live = (position >= span_first) & (position <= span_last)
        values_t = lax.dot_general(
            wv_ref[...], latent, (((0,), (1,)), ((), ())), preferred_element_type=jnp.float32
        ).astype(jnp.bfloat16)
        for h in range(heads):
            keys = jnp.dot(
                latent, wk_ref[:, h * HEAD_LANES : (h + 1) * HEAD_LANES],
                preferred_element_type=jnp.float32,
            ).astype(jnp.bfloat16) + extra
            scores = lax.dot_general(
                keys, turned[h], (((1,), (1,)), ((), ())), preferred_element_type=jnp.float32
            ) * scale
            scores = jnp.where(live, scores, -1e30)
            old = high[h : h + 1, :]
            new = jnp.maximum(old, jnp.max(scores, axis=0, keepdims=True))
            weights = jnp.where(live, jnp.exp(scores - new), 0.0)
            factor = jnp.exp(old - new)
            high[h : h + 1, :] = new
            total[h : h + 1, :] = total[h : h + 1, :] * factor + jnp.sum(
                weights, axis=0, keepdims=True
            )
            acc[h] = acc[h] * factor + jnp.dot(
                values_t[h * VALUE_ENTRIES : (h + 1) * VALUE_ENTRIES],
                weights.astype(jnp.bfloat16),
                preferred_element_type=jnp.float32,
            )
        return carry

    lax.fori_loop(lo_ref[0], lo_ref[1], step, 0)
    for h in range(heads):
        out_ref[h * VALUE_ENTRIES : (h + 1) * VALUE_ENTRIES, :] = (
            acc[h] / total[h : h + 1, :]
        ).astype(jnp.bfloat16)


def attend(queries, packed, doc_ids, latent_to_key, latent_to_value, positions, cosine, sine):
    rows = queries.shape[0]
    heads = queries.shape[1] // (UNROTATED_DIM + ROPE)
    rank = latent_to_key.shape[0]
    count = packed.shape[0]
    docs = packed[:, rank + UNROTATED_DIM + ROPE].astype(jnp.int32)
    starts = jnp.sum((docs[:, None] < doc_ids[None, :]).astype(jnp.int32), axis=0)
    block = math.gcd(count, 256)
    bounds = jnp.stack([starts[0] // block, positions[-1] // block + 1]).astype(jnp.int32)
    span = jnp.stack([starts, positions])
    one, none = jnp.ones((rows, UNROTATED_DIM)), jnp.zeros((rows, HEAD_LANES - UNROTATED_DIM - ROPE))
    table = jnp.concatenate(
        [one, cosine, cosine, none, 0.0 * one, sine, sine, none], axis=1
    ).astype(jnp.float32)
    wk = jnp.pad(
        latent_to_key.reshape(rank, heads, UNROTATED_DIM),
        ((0, 0), (0, 0), (0, HEAD_LANES - UNROTATED_DIM)),
    ).reshape(rank, heads * HEAD_LANES)
    vmem = pl.BlockSpec(memory_space=pltpu.VMEM)
    out = pl.pallas_call(
        functools.partial(attention_kernel, heads, block),
        out_shape=jax.ShapeDtypeStruct((heads * VALUE_ENTRIES, rows), jnp.bfloat16),
        in_specs=[pl.BlockSpec(memory_space=pltpu.SMEM)] + [vmem] * 6,
        out_specs=vmem,
        scratch_shapes=[
            pltpu.VMEM((heads, rows, HEAD_LANES), jnp.bfloat16),
            pltpu.VMEM((heads, rows), jnp.float32),
            pltpu.VMEM((heads, rows), jnp.float32),
            pltpu.VMEM((heads, VALUE_ENTRIES, rows), jnp.float32),
        ],
        compiler_params=pltpu.CompilerParams(vmem_limit_bytes=40 * 1024 * 1024),
        name="attend",
    )(bounds, queries, table, span, packed, wk, latent_to_value)
    return out.T


def local(
    residual,
    queries,
    latent,
    rope_key,
    doc_ids,
    latent_to_key,
    latent_to_value,
    out_proj,
    mix_gain,
    moe_gain,
    expert_ids,
    route_weight,
    gate_weight,
    up_weight,
    down_weight,
):
    local_rows = queries.shape[0]
    positions = lax.axis_index("sp") * local_rows + jnp.arange(local_rows, dtype=jnp.int32)
    cosine, sine = angles_of(positions)
    half = ROPE // 2
    upper, lower = rope_key[:, :half].astype(jnp.float32), rope_key[:, half:].astype(jnp.float32)
    key_rot = jnp.concatenate(
        [upper * cosine - lower * sine, lower * cosine + upper * sine], axis=1
    ).astype(jnp.bfloat16)
    own = jnp.concatenate(
        [
            latent,
            jnp.zeros((local_rows, UNROTATED_DIM), jnp.bfloat16),
            key_rot,
            doc_ids.astype(jnp.bfloat16)[:, None],
            jnp.zeros((local_rows, HEAD_LANES - UNROTATED_DIM - ROPE - 1), jnp.bfloat16),
        ],
        axis=1,
    )
    packed = lax.all_gather(own, "sp", axis=0, tiled=True)
    attended = attend(
        queries, packed, doc_ids, latent_to_key, latent_to_value, positions, cosine, sine
    )
    gathered = lax.all_to_all(attended, "tp", split_axis=0, concat_axis=1, tiled=True)
    mix = jnp.dot(gathered, out_proj, preferred_element_type=jnp.float32)
    branch = rms_scale(mix, mix_gain)
    middle = lax.optimization_barrier((residual.astype(jnp.float32) + branch).astype(jnp.bfloat16))
    normed = rms_scale(middle.astype(jnp.float32), moe_gain).astype(jnp.bfloat16)
    row_count = normed.shape[0]
    width = normed.shape[1]
    top_count = expert_ids.shape[1]
    expert_count = lax.axis_size("sp")
    capacity = row_count // (expert_count // GROUPS)
    flat_ids = expert_ids.reshape(-1)
    onehot = (flat_ids[:, None] == jnp.arange(expert_count, dtype=jnp.int32)[None, :]).astype(
        jnp.int32
    )
    earlier = jnp.cumsum(onehot, axis=0) - onehot
    slot_rank = jnp.sum(earlier * onehot, axis=1)
    slot_ids = (flat_ids * capacity + slot_rank).reshape(row_count, top_count)
    matches = (
        slot_ids[:, :, None]
        == jnp.arange(expert_count * capacity, dtype=jnp.int32)[None, None, :]
    )
    chooser = jnp.any(matches, axis=1).astype(jnp.bfloat16)
    buffer = lax.dot_general(
        chooser, normed, (((0,), (0,)), ((), ())), preferred_element_type=jnp.float32
    ).astype(jnp.bfloat16)
    buffer = buffer.reshape(expert_count, capacity, width)
    arrived = lax.all_to_all(buffer, "sp", split_axis=0, concat_axis=0, tiled=True)
    both_halves = lax.all_gather(arrived, "tp", axis=0, tiled=True)
    flat_rows = both_halves.reshape(-1, width)
    gate_out = jnp.dot(flat_rows, gate_weight[0], preferred_element_type=jnp.float32)
    upward = jnp.dot(flat_rows, up_weight[0], preferred_element_type=jnp.float32)
    hidden = (jax.nn.silu(gate_out) * upward).astype(jnp.bfloat16)
    partial_value = jnp.dot(hidden, down_weight[0], preferred_element_type=jnp.float32).reshape(
        both_halves.shape
    )
    summed = lax.psum_scatter(
        partial_value.astype(jnp.bfloat16), "tp", scatter_dimension=0, tiled=True
    )
    returned = lax.all_to_all(summed, "sp", split_axis=0, concat_axis=0, tiled=True)
    share = jnp.sum(jnp.where(matches, route_weight[:, :, None], 0.0), axis=1)
    coarse = share.astype(jnp.bfloat16)
    fine = (share - coarse.astype(jnp.float32)).astype(jnp.bfloat16)
    flat = returned.reshape(-1, width)
    expert_mix = jnp.dot(coarse, flat, preferred_element_type=jnp.float32) + jnp.dot(
        fine, flat, preferred_element_type=jnp.float32
    )
    return (middle.astype(jnp.float32) + expert_mix).astype(jnp.bfloat16)


def solution(mesh):
    in_specs = (
        P(("sp", "tp"), None),
        P("sp", "tp"),
        P("sp", None),
        P("sp", None),
        P("sp"),
        P(None, "tp"),
        P(None, "tp"),
        P(),
        P(),
        P(),
        P(("sp", "tp"), None),
        P(("sp", "tp"), None),
        P("sp", None, "tp"),
        P("sp", None, "tp"),
        P("sp", "tp", None),
    )
    out_specs = P(("sp", "tp"), None)
    return jax.shard_map(local, mesh=mesh, in_specs=in_specs, out_specs=out_specs, check_vma=False)
```

```python
import functools
import math

import jax
import jax.numpy as jnp
from jax import lax
from jax.experimental import pallas as pl
from jax.experimental.pallas import tpu as pltpu
from jax.sharding import PartitionSpec as P

UNROTATED_DIM = 64
ROPE = 32
VALUE_ENTRIES = 64
GROUPS = 4
HEAD_LANES = 128
MESH = pl.DeviceIdType.MESH

rope_base = 10000.0
epsilon = 1e-06


def angles_of(positions):
    half_width = ROPE // 2
    frequency = rope_base ** (-jnp.arange(half_width, dtype=jnp.float32) / half_width)
    angles = positions.astype(jnp.float32)[:, None] * frequency[None, :]
    return jnp.cos(angles), jnp.sin(angles)


def rms_scale(source, gain):
    return source * lax.rsqrt(jnp.mean(source * source, axis=-1, keepdims=True) + epsilon) * gain


def attention_kernel(
    heads, block, lo_ref, query_ref, table_ref, span_ref, packed_ref, wk_ref, wv_ref, out_ref,
    turned, high, total, acc,
):
    rows = query_ref.shape[0]
    width = query_ref.shape[1]
    rank = wk_ref.shape[0]
    per_head = UNROTATED_DIM + ROPE
    cosine = table_ref[:, :HEAD_LANES]
    sine = table_ref[:, HEAD_LANES:]
    for h in range(heads):
        first = h * per_head // 128 * 128
        last = min(-(-(h + 1) * per_head // 128) * 128, width)
        window = query_ref[:, first:last]
        shape = (last - first, HEAD_LANES)
        source = lax.broadcasted_iota(jnp.int32, shape, 0) + (first - h * per_head)
        lane = lax.broadcasted_iota(jnp.int32, shape, 1)
        half = ROPE // 2
        plain = jnp.where((source == lane) & (lane < per_head), 1.0, 0.0).astype(jnp.bfloat16)
        upper = (lane >= UNROTATED_DIM) & (lane < UNROTATED_DIM + half) & (source == lane + half)
        lower = (lane >= UNROTATED_DIM + half) & (lane < per_head) & (source == lane - half)
        crossed = (jnp.where(lower, 1.0, 0.0) - jnp.where(upper, 1.0, 0.0)).astype(jnp.bfloat16)
        straight = jnp.dot(window, plain, preferred_element_type=jnp.float32)
        swapped = jnp.dot(window, crossed, preferred_element_type=jnp.float32)
        turned[h] = (straight * cosine + swapped * sine).astype(jnp.bfloat16)
    high[...] = jnp.full(high.shape, -1e30, jnp.float32)
    total[...] = jnp.zeros(total.shape, jnp.float32)
    acc[...] = jnp.zeros(acc.shape, jnp.float32)
    span_first = span_ref[0:1, :]
    span_last = span_ref[1:2, :]
    scale = per_head ** (-0.5)

    def step(number, carry):
        base = pl.multiple_of(number * block, block)
        latent = packed_ref[pl.ds(base, block), :rank]
        extra = packed_ref[pl.ds(base, block), rank:]
        position = base + lax.broadcasted_iota(jnp.int32, (block, rows), 0)
        live = (position >= span_first) & (position <= span_last)
        values_t = lax.dot_general(
            wv_ref[...], latent, (((0,), (1,)), ((), ())), preferred_element_type=jnp.float32
        ).astype(jnp.bfloat16)
        for h in range(heads):
            keys = jnp.dot(
                latent, wk_ref[:, h * HEAD_LANES : (h + 1) * HEAD_LANES],
                preferred_element_type=jnp.float32,
            ).astype(jnp.bfloat16) + extra
            scores = lax.dot_general(
                keys, turned[h], (((1,), (1,)), ((), ())), preferred_element_type=jnp.float32
            ) * scale
            scores = jnp.where(live, scores, -1e30)
            old = high[h : h + 1, :]
            new = jnp.maximum(old, jnp.max(scores, axis=0, keepdims=True))
            weights = jnp.where(live, jnp.exp(scores - new), 0.0)
            factor = jnp.exp(old - new)
            high[h : h + 1, :] = new
            total[h : h + 1, :] = total[h : h + 1, :] * factor + jnp.sum(
                weights, axis=0, keepdims=True
            )
            acc[h] = acc[h] * factor + jnp.dot(
                values_t[h * VALUE_ENTRIES : (h + 1) * VALUE_ENTRIES],
                weights.astype(jnp.bfloat16),
                preferred_element_type=jnp.float32,
            )
        return carry

    lax.fori_loop(lo_ref[0], lo_ref[1], step, 0)
    for h in range(heads):
        out_ref[h * VALUE_ENTRIES : (h + 1) * VALUE_ENTRIES, :] = (
            acc[h] / total[h : h + 1, :]
        ).astype(jnp.bfloat16)


def attend(queries, packed, doc_ids, latent_to_key, latent_to_value, positions, cosine, sine):
    rows = queries.shape[0]
    heads = queries.shape[1] // (UNROTATED_DIM + ROPE)
    rank = latent_to_key.shape[0]
    count = packed.shape[0]
    docs = packed[:, rank + UNROTATED_DIM + ROPE].astype(jnp.int32)
    starts = jnp.sum((docs[:, None] < doc_ids[None, :]).astype(jnp.int32), axis=0)
    block = math.gcd(count, 256)
    bounds = jnp.stack([starts[0] // block, positions[-1] // block + 1]).astype(jnp.int32)
    span = jnp.stack([starts, positions])
    one, none = jnp.ones((rows, UNROTATED_DIM)), jnp.zeros((rows, HEAD_LANES - UNROTATED_DIM - ROPE))
    table = jnp.concatenate(
        [one, cosine, cosine, none, 0.0 * one, sine, sine, none], axis=1
    ).astype(jnp.float32)
    wk = jnp.pad(
        latent_to_key.reshape(rank, heads, UNROTATED_DIM),
        ((0, 0), (0, 0), (0, HEAD_LANES - UNROTATED_DIM)),
    ).reshape(rank, heads * HEAD_LANES)
    vmem = pl.BlockSpec(memory_space=pltpu.VMEM)
    out = pl.pallas_call(
        functools.partial(attention_kernel, heads, block),
        out_shape=jax.ShapeDtypeStruct((heads * VALUE_ENTRIES, rows), jnp.bfloat16),
        in_specs=[pl.BlockSpec(memory_space=pltpu.SMEM)] + [vmem] * 6,
        out_specs=vmem,
        scratch_shapes=[
            pltpu.VMEM((heads, rows, HEAD_LANES), jnp.bfloat16),
            pltpu.VMEM((heads, rows), jnp.float32),
            pltpu.VMEM((heads, rows), jnp.float32),
            pltpu.VMEM((heads, VALUE_ENTRIES, rows), jnp.float32),
        ],
        compiler_params=pltpu.CompilerParams(vmem_limit_bytes=40 * 1024 * 1024),
        name="attend",
    )(bounds, queries, table, span, packed, wk, latent_to_value)
    return out.T


def greet(groups, plane):
    index, core = lax.axis_index("sp"), lax.axis_index("tp")
    level, place = index // plane, lax.rem(index, plane)
    barrier = pltpu.get_barrier_semaphore()
    peers = [(lax.rem(level + d, groups) * plane + place, core) for d in range(1, groups)]
    peers += [(level * plane + lax.rem(place + d, plane), core) for d in range(1, plane)]
    peers += [(index, 1 - core)]
    for peer in peers:
        pl.semaphore_signal(barrier, inc=1, device_id=peer, device_id_type=MESH)
    pl.semaphore_wait(barrier, len(peers))
    return index, core, level, place


def remote(source, target, send_sem, recv_sem, peer):
    return pltpu.make_async_remote_copy(
        src_ref=source, dst_ref=target, send_sem=send_sem, recv_sem=recv_sem,
        device_id=peer, device_id_type=MESH,
    )


def level_order(groups):
    return sorted(range(groups), key=lambda d: min(d, groups - d))


def dispatch_kernel(
    groups, plane, capacity, rows_ref, meta_ref, out_ref, metas_ref,
    landed, spread, z_send, z_recv, m_send, m_recv, p_send, p_recv, t_send, t_recv, own_sem,
):
    index, core, level, place = greet(groups, plane)
    started = []
    for d in sorted(range(1, groups), key=lambda d: -min(d, groups - d)):
        other = lax.rem(level + d, groups)
        peer = (other * plane + place, core)
        first = remote(
            meta_ref.at[other], metas_ref.at[level], m_send.at[d], m_recv.at[level], peer
        )
        second = remote(
            rows_ref.at[other], landed.at[level], z_send.at[d], z_recv.at[level], peer
        )
        first.start()
        second.start()
        started += [first, second]
    metas_ref[level] = meta_ref[level]
    slots = plane * capacity
    group_rows = rows_ref.shape[1]
    locals_ = []
    for d in level_order(groups):
        source = lax.rem(level + groups - d, groups)
        if d == 0:
            rows, info = rows_ref[level], meta_ref[level]
        else:
            peer = (source * plane + place, core)
            remote(meta_ref.at[source], metas_ref.at[source], m_send.at[d], m_recv.at[source], peer).wait_recv()
            remote(rows_ref.at[source], landed.at[source], z_send.at[d], z_recv.at[source], peer).wait_recv()
            rows, info = landed[source], metas_ref[source]
        info = info[:, :group_rows].astype(jnp.float32)
        slot = lax.broadcasted_iota(jnp.int32, (slots, group_rows), 0).astype(jnp.float32)
        chooser = jnp.where((slot == info[0:1]) | (slot == info[1:2]), 1.0, 0.0)
        picked = jnp.dot(chooser.astype(jnp.bfloat16), rows, preferred_element_type=jnp.float32)
        for e in range(plane):
            spread[d, e] = picked[e * capacity : (e + 1) * capacity].astype(jnp.bfloat16)
        for far in range(plane - 1, 0, -1):
            to = lax.rem(place + far, plane)
            copy = remote(
                spread.at[d, to], out_ref.at[core, source, place],
                p_send.at[d * plane + far], p_recv.at[source * plane + place],
                (level * plane + to, core),
            )
            copy.start()
            started.append(copy)
        keep = pltpu.make_async_copy(
            spread.at[d, place], out_ref.at[core, source, place], own_sem.at[d]
        )
        keep.start()
        locals_.append(keep)
    for at, d in enumerate(level_order(groups)):
        source = lax.rem(level + groups - d, groups)
        for far in range(1, plane):
            origin = lax.rem(place + plane - far, plane)
            remote(
                spread.at[d, origin], out_ref.at[core, source, origin],
                p_send.at[d * plane + far], p_recv.at[source * plane + origin],
                (level * plane + origin, core),
            ).wait_recv()
        locals_[at].wait()
        copy = remote(
            out_ref.at[core, source], out_ref.at[core, source],
            t_send.at[d], t_recv.at[source], (index, 1 - core),
        )
        copy.start()
        started.append(copy)
    for d in level_order(groups):
        source = lax.rem(level + groups - d, groups)
        remote(
            out_ref.at[1 - core, source], out_ref.at[1 - core, source],
            t_send.at[d], t_recv.at[source], (index, 1 - core),
        ).wait_recv()
    for copy in started:
        copy.wait_send()


def return_kernel(
    groups, plane, capacity, part_ref, metas_ref, out_ref,
    passed, mixed, back, merged, t_send, t_recv, p_send, p_recv, own_sem, z_send, z_recv,
):
    index, core, level, place = greet(groups, plane)
    started, locals_ = [], []
    order = level_order(groups)[::-1]
    slots = plane * capacity
    group_rows = out_ref.shape[1]
    for d in order:
        goal = lax.rem(level + d, groups)
        copy = remote(
            part_ref.at[1 - core, goal], passed.at[goal], t_send.at[d], t_recv.at[goal],
            (index, 1 - core),
        )
        copy.start()
        started.append(copy)
    for d in order:
        goal = lax.rem(level + d, groups)
        remote(
            part_ref.at[core, goal], passed.at[goal], t_send.at[d], t_recv.at[goal],
            (index, 1 - core),
        ).wait_recv()
        for e in range(plane):
            mixed[d, e] = (
                part_ref[core, goal, e].astype(jnp.float32) + passed[goal, e].astype(jnp.float32)
            ).astype(jnp.bfloat16)
        for far in range(plane - 1, 0, -1):
            to = lax.rem(place + far, plane)
            copy = remote(
                mixed.at[d, to], back.at[goal, place],
                p_send.at[d * plane + far], p_recv.at[goal * plane + place],
                (level * plane + to, core),
            )
            copy.start()
            started.append(copy)
        keep = pltpu.make_async_copy(mixed.at[d, place], back.at[goal, place], own_sem.at[d])
        keep.start()
        locals_.append(keep)
    for at, d in enumerate(order):
        goal = lax.rem(level + d, groups)
        for far in range(1, plane):
            origin = lax.rem(place + plane - far, plane)
            remote(
                mixed.at[d, origin], back.at[goal, origin],
                p_send.at[d * plane + far], p_recv.at[goal * plane + origin],
                (level * plane + origin, core),
            ).wait_recv()
        locals_[at].wait()
        info = metas_ref[goal][:, :group_rows].astype(jnp.float32)
        slot = lax.broadcasted_iota(jnp.int32, (slots, group_rows), 0).astype(jnp.float32)
        hit_first, hit_second = slot == info[0:1], slot == info[1:2]
        arrived = back[goal].reshape(slots, back.shape[-1])
        result = 0.0
        for term in range(2):
            share = jnp.where(hit_first, info[2 + term : 3 + term], 0.0) + jnp.where(
                hit_second, info[4 + term : 5 + term], 0.0
            )
            result = result + lax.dot_general(
                share.astype(jnp.bfloat16), arrived, (((0,), (0,)), ((), ())),
                preferred_element_type=jnp.float32,
            )
        if d == 0:
            out_ref[level] = result.astype(jnp.bfloat16)
        else:
            merged[d] = result.astype(jnp.bfloat16)
            copy = remote(
                merged.at[d], out_ref.at[level], z_send.at[d], z_recv.at[level],
                (goal * plane + place, core),
            )
            copy.start()
            started.append(copy)
    for d in range(1, groups):
        other = lax.rem(level + groups - d, groups)
        remote(
            merged.at[d], out_ref.at[other], z_send.at[d], z_recv.at[other],
            (other * plane + place, core),
        ).wait_recv()
    for copy in started:
        copy.wait_send()


def dispatch(rows, meta, plane, capacity):
    groups, group_rows, width = rows.shape
    vmem = pl.BlockSpec(memory_space=pltpu.VMEM)
    dma = pltpu.SemaphoreType.DMA
    few, many = dma((groups,)), dma((groups * plane,))
    return pl.pallas_call(
        functools.partial(dispatch_kernel, groups, plane, capacity),
        out_shape=(
            jax.ShapeDtypeStruct((2, groups, plane, capacity, width), jnp.bfloat16),
            jax.ShapeDtypeStruct(meta.shape, jnp.bfloat16),
        ),
        in_specs=[vmem, vmem],
        out_specs=(vmem, vmem),
        scratch_shapes=[
            pltpu.VMEM((groups, group_rows, width), jnp.bfloat16),
            pltpu.VMEM((groups, plane, capacity, width), jnp.bfloat16),
            few, few, few, few, many, many, few, few, few,
        ],
        compiler_params=pltpu.CompilerParams(
            collective_id=1, has_side_effects=True, vmem_limit_bytes=40 * 1024 * 1024
        ),
        name="dispatch",
    )(rows, meta)


def give_back(partial_value, metas, group_rows):
    _, groups, plane, capacity, width = partial_value.shape
    vmem = pl.BlockSpec(memory_space=pltpu.VMEM)
    dma = pltpu.SemaphoreType.DMA
    few, many = dma((groups,)), dma((groups * plane,))
    block = pltpu.VMEM((groups, plane, capacity, width), jnp.bfloat16)
    return pl.pallas_call(
        functools.partial(return_kernel, groups, plane, capacity),
        out_shape=jax.ShapeDtypeStruct((groups, group_rows, width), jnp.bfloat16),
        in_specs=[vmem, vmem],
        out_specs=vmem,
        scratch_shapes=[
            block, block, block,
            pltpu.VMEM((groups, group_rows, width), jnp.bfloat16),
            few, few, many, many, few, few, few,
        ],
        compiler_params=pltpu.CompilerParams(
            collective_id=2, has_side_effects=True, vmem_limit_bytes=40 * 1024 * 1024
        ),
        name="give_back",
    )(partial_value, metas)


def local(
    residual,
    queries,
    latent,
    rope_key,
    doc_ids,
    latent_to_key,
    latent_to_value,
    out_proj,
    mix_gain,
    moe_gain,
    expert_ids,
    route_weight,
    gate_weight,
    up_weight,
    down_weight,
):
    local_rows = queries.shape[0]
    positions = lax.axis_index("sp") * local_rows + jnp.arange(local_rows, dtype=jnp.int32)
    cosine, sine = angles_of(positions)
    half = ROPE // 2
    upper, lower = rope_key[:, :half].astype(jnp.float32), rope_key[:, half:].astype(jnp.float32)
    key_rot = jnp.concatenate(
        [upper * cosine - lower * sine, lower * cosine + upper * sine], axis=1
    ).astype(jnp.bfloat16)
    own = jnp.concatenate(
        [
            latent,
            jnp.zeros((local_rows, UNROTATED_DIM), jnp.bfloat16),
            key_rot,
            doc_ids.astype(jnp.bfloat16)[:, None],
            jnp.zeros((local_rows, HEAD_LANES - UNROTATED_DIM - ROPE - 1), jnp.bfloat16),
        ],
        axis=1,
    )
    packed = lax.all_gather(own, "sp", axis=0, tiled=True)
    attended = attend(
        queries, packed, doc_ids, latent_to_key, latent_to_value, positions, cosine, sine
    )
    gathered = lax.all_to_all(attended, "tp", split_axis=0, concat_axis=1, tiled=True)
    mix = jnp.dot(gathered, out_proj, preferred_element_type=jnp.float32)
    branch = rms_scale(mix, mix_gain)
    middle = lax.optimization_barrier((residual.astype(jnp.float32) + branch).astype(jnp.bfloat16))
    normed = rms_scale(middle.astype(jnp.float32), moe_gain).astype(jnp.bfloat16)
    row_count = normed.shape[0]
    width = normed.shape[1]
    top_count = expert_ids.shape[1]
    expert_count = lax.axis_size("sp")
    capacity = row_count // (expert_count // GROUPS)
    flat_ids = expert_ids.reshape(-1)
    onehot = (flat_ids[:, None] == jnp.arange(expert_count, dtype=jnp.int32)[None, :]).astype(
        jnp.int32
    )
    earlier = jnp.cumsum(onehot, axis=0) - onehot
    slot_rank = jnp.sum(earlier * onehot, axis=1)
    plane = expert_count // GROUPS
    group_rows = capacity * plane // top_count
    group_of = expert_ids[:, 0] // plane
    in_group = (group_of[:, None] == jnp.arange(GROUPS, dtype=jnp.int32)[None, :]).astype(jnp.int32)
    group_rank = jnp.sum((jnp.cumsum(in_group, axis=0) - in_group) * in_group, axis=1)
    slots = (lax.rem(flat_ids, plane) * capacity + slot_rank).reshape(row_count, top_count)
    member = (group_of * group_rows + group_rank)[:, None]
    chooser = (member == jnp.arange(GROUPS * group_rows, dtype=jnp.int32)[None, :]).astype(
        jnp.bfloat16
    )
    coarse = route_weight.astype(jnp.bfloat16)
    fine = (route_weight - coarse.astype(jnp.float32)).astype(jnp.bfloat16)
    fields = jnp.concatenate(
        [
            (slots + 1).astype(jnp.bfloat16),
            jnp.stack([coarse[:, 0], fine[:, 0], coarse[:, 1], fine[:, 1]], axis=1),
        ],
        axis=1,
    )
    fields = jnp.pad(fields, ((0, 0), (0, 16 - fields.shape[1])))
    meta = lax.dot_general(
        fields, chooser, (((0,), (0,)), ((), ())), preferred_element_type=jnp.float32
    )
    meta = meta - (jnp.arange(16) < top_count)[:, None].astype(jnp.float32)
    meta = meta.astype(jnp.bfloat16).reshape(16, GROUPS, group_rows).transpose(1, 0, 2)
    meta = jnp.pad(meta, ((0, 0), (0, 0), (0, -group_rows % 128)))
    grouped = lax.dot_general(
        chooser, normed, (((0,), (0,)), ((), ())), preferred_element_type=jnp.float32
    ).astype(jnp.bfloat16)
    arrived, metas = dispatch(
        grouped.reshape(GROUPS, group_rows, width), meta, plane, capacity
    )
    flat_rows = arrived.reshape(-1, width)
    gate_out = jnp.dot(flat_rows, gate_weight[0], preferred_element_type=jnp.float32)
    upward = jnp.dot(flat_rows, up_weight[0], preferred_element_type=jnp.float32)
    hidden = (jax.nn.silu(gate_out) * upward).astype(jnp.bfloat16)
    partial_value = jnp.dot(hidden, down_weight[0], preferred_element_type=jnp.float32)
    returned = give_back(
        partial_value.astype(jnp.bfloat16).reshape(arrived.shape), metas, group_rows
    )
    expert_mix = jnp.dot(
        chooser, returned.reshape(-1, width), preferred_element_type=jnp.float32
    )
    return (middle.astype(jnp.float32) + expert_mix).astype(jnp.bfloat16)


def solution(mesh):
    in_specs = (
        P(("sp", "tp"), None),
        P("sp", "tp"),
        P("sp", None),
        P("sp", None),
        P("sp"),
        P(None, "tp"),
        P(None, "tp"),
        P(),
        P(),
        P(),
        P(("sp", "tp"), None),
        P(("sp", "tp"), None),
        P("sp", None, "tp"),
        P("sp", None, "tp"),
        P("sp", "tp", None),
    )
    out_specs = P(("sp", "tp"), None)
    return jax.shard_map(local, mesh=mesh, in_specs=in_specs, out_specs=out_specs, check_vma=False)
```

```python
import functools
import math

import jax
import jax.numpy as jnp
from jax import lax
from jax.experimental import pallas as pl
from jax.experimental.pallas import tpu as pltpu
from jax.sharding import PartitionSpec as P

UNROTATED_DIM = 64
ROPE = 32
VALUE_ENTRIES = 64
GROUPS = 4
HEAD_LANES = 128
MESH = pl.DeviceIdType.MESH

rope_base = 10000.0
epsilon = 1e-06


def angles_of(positions):
    half_width = ROPE // 2
    frequency = rope_base ** (-jnp.arange(half_width, dtype=jnp.float32) / half_width)
    lane = jnp.arange(HEAD_LANES)
    turns = (lane >= UNROTATED_DIM) & (lane < UNROTATED_DIM + ROPE)
    frequency = jnp.where(turns, jnp.tile(frequency, HEAD_LANES // half_width), 0.0)
    angles = positions.astype(jnp.float32)[:, None] * frequency[None, :]
    return jnp.cos(angles), jnp.sin(angles)


def rms_scale(source, gain):
    return source * lax.rsqrt(jnp.mean(source * source, axis=-1, keepdims=True) + epsilon) * gain


def attention_kernel(
    heads, block, lo_ref, query_ref, cos_ref, sin_ref, span_ref, packed_ref, wk_ref, wv_ref, out_ref,
    turned, wide, high, total, acc,
):
    rows = query_ref.shape[0]
    width = query_ref.shape[1]
    rank = wk_ref.shape[0]
    per_head = UNROTATED_DIM + ROPE
    cosine = cos_ref[...]
    sine = sin_ref[...]
    for h in range(heads):
        first = h * per_head // 128 * 128
        last = min(-(-(h + 1) * per_head // 128) * 128, width)
        window = query_ref[:, first:last]
        shape = (last - first, HEAD_LANES)
        source = lax.broadcasted_iota(jnp.int32, shape, 0) + (first - h * per_head)
        lane = lax.broadcasted_iota(jnp.int32, shape, 1)
        half = ROPE // 2
        plain = jnp.where((source == lane) & (lane < per_head), 1.0, 0.0).astype(jnp.bfloat16)
        upper = (lane >= UNROTATED_DIM) & (lane < UNROTATED_DIM + half) & (source == lane + half)
        lower = (lane >= UNROTATED_DIM + half) & (lane < per_head) & (source == lane - half)
        crossed = (jnp.where(lower, 1.0, 0.0) - jnp.where(upper, 1.0, 0.0)).astype(jnp.bfloat16)
        straight = jnp.dot(window, plain, preferred_element_type=jnp.float32)
        swapped = jnp.dot(window, crossed, preferred_element_type=jnp.float32)
        low = h * UNROTATED_DIM // HEAD_LANES * HEAD_LANES
        pair = wk_ref[:, low : low + HEAD_LANES].astype(jnp.float32)
        if h * UNROTATED_DIM > low:
            pair = pltpu.roll(pair, HEAD_LANES - (h * UNROTATED_DIM - low), 1)
        column = lax.broadcasted_iota(jnp.int32, pair.shape, 1)
        wide[h] = jnp.where(column < UNROTATED_DIM, pair, 0.0).astype(jnp.bfloat16)
        turned[h] = (straight * cosine + swapped * sine).astype(jnp.bfloat16)
    high[...] = jnp.full(high.shape, -1e30, jnp.float32)
    total[...] = jnp.zeros(total.shape, jnp.float32)
    acc[...] = jnp.zeros(acc.shape, jnp.float32)
    span_first = span_ref[0:1, :]
    span_last = span_ref[1:2, :]
    scale = per_head ** (-0.5)

    def step(number, carry):
        base = pl.multiple_of(number * block, block)
        latent = packed_ref[pl.ds(base, block), :rank]
        extra = packed_ref[pl.ds(base, block), rank:]
        position = base + lax.broadcasted_iota(jnp.int32, (block, rows), 0)
        live = (position >= span_first) & (position <= span_last)
        values_t = lax.dot_general(
            wv_ref[...], latent, (((0,), (1,)), ((), ())), preferred_element_type=jnp.float32
        ).astype(jnp.bfloat16)
        for h in range(heads):
            keys = jnp.dot(
                latent, wide[h],
                preferred_element_type=jnp.float32,
            ).astype(jnp.bfloat16) + extra
            scores = lax.dot_general(
                keys, turned[h], (((1,), (1,)), ((), ())), preferred_element_type=jnp.float32
            ) * scale
            scores = jnp.where(live, scores, -1e30)
            old = high[h : h + 1, :]
            new = jnp.maximum(old, jnp.max(scores, axis=0, keepdims=True))
            weights = jnp.where(live, jnp.exp(scores - new), 0.0)
            factor = jnp.exp(old - new)
            high[h : h + 1, :] = new
            total[h : h + 1, :] = total[h : h + 1, :] * factor + jnp.sum(
                weights, axis=0, keepdims=True
            )
            acc[h] = acc[h] * factor + jnp.dot(
                values_t[h * VALUE_ENTRIES : (h + 1) * VALUE_ENTRIES],
                weights.astype(jnp.bfloat16),
                preferred_element_type=jnp.float32,
            )
        return carry

    lax.fori_loop(lo_ref[0], lo_ref[1], step, 0)
    for h in range(heads):
        out_ref[h * VALUE_ENTRIES : (h + 1) * VALUE_ENTRIES, :] = (
            acc[h] / total[h : h + 1, :]
        ).astype(jnp.bfloat16)


def attend(queries, packed, doc_ids, latent_to_key, latent_to_value, positions, cosine, sine):
    rows = queries.shape[0]
    heads = queries.shape[1] // (UNROTATED_DIM + ROPE)
    rank = latent_to_key.shape[0]
    count = packed.shape[0]
    place = jnp.arange(count, dtype=jnp.int32)
    docs = packed[:, rank + UNROTATED_DIM + ROPE].astype(jnp.int32)
    docs = jnp.where(place < positions[0] - count // 2, -1, docs)
    docs = jnp.where(place > positions[-1], jnp.iinfo(jnp.int32).max, docs)
    starts = jnp.sum((docs[:, None] < doc_ids[None, :]).astype(jnp.int32), axis=0)
    block = math.gcd(count, 256)
    bounds = jnp.stack([starts[0] // block, positions[-1] // block + 1]).astype(jnp.int32)
    span = jnp.stack([starts, positions])
    vmem = pl.BlockSpec(memory_space=pltpu.VMEM)
    out = pl.pallas_call(
        functools.partial(attention_kernel, heads, block),
        out_shape=jax.ShapeDtypeStruct((heads * VALUE_ENTRIES, rows), jnp.bfloat16),
        in_specs=[pl.BlockSpec(memory_space=pltpu.SMEM)] + [vmem] * 7,
        out_specs=vmem,
        scratch_shapes=[
            pltpu.VMEM((heads, rows, HEAD_LANES), jnp.bfloat16),
            pltpu.VMEM((heads, rank, HEAD_LANES), jnp.bfloat16),
            pltpu.VMEM((heads, rows), jnp.float32),
            pltpu.VMEM((heads, rows), jnp.float32),
            pltpu.VMEM((heads, VALUE_ENTRIES, rows), jnp.float32),
        ],
        compiler_params=pltpu.CompilerParams(vmem_limit_bytes=40 * 1024 * 1024),
        name="attend",
    )(bounds, queries, cosine, sine, span, packed, latent_to_key, latent_to_value)
    return out.T


def greet(groups, plane):
    index, core = lax.axis_index("sp"), lax.axis_index("tp")
    level, place = index // plane, lax.rem(index, plane)
    barrier = pltpu.get_barrier_semaphore()
    peers = [(lax.rem(level + d, groups) * plane + place, core) for d in range(1, groups)]
    peers += [(level * plane + lax.rem(place + d, plane), core) for d in range(1, plane)]
    peers += [(index, 1 - core)]
    for peer in peers:
        pl.semaphore_signal(barrier, inc=1, device_id=peer, device_id_type=MESH)
    pl.semaphore_wait(barrier, len(peers))
    return index, core, level, place


def remote(source, target, send_sem, recv_sem, peer):
    return pltpu.make_async_remote_copy(
        src_ref=source, dst_ref=target, send_sem=send_sem, recv_sem=recv_sem,
        device_id=peer, device_id_type=MESH,
    )


def level_order(groups):
    return sorted(range(groups), key=lambda d: min(d, groups - d))


def dispatch_kernel(
    groups, plane, capacity, rows_ref, meta_ref, out_ref, metas_ref,
    landed, spread, z_send, z_recv, m_send, m_recv, p_send, p_recv, t_send, t_recv, own_sem,
):
    index, core, level, place = greet(groups, plane)
    started = []
    for d in sorted(range(1, groups), key=lambda d: -min(d, groups - d)):
        other = lax.rem(level + d, groups)
        peer = (other * plane + place, core)
        first = remote(
            meta_ref.at[other], metas_ref.at[level], m_send.at[d], m_recv.at[level], peer
        )
        second = remote(
            rows_ref.at[other], landed.at[level], z_send.at[d], z_recv.at[level], peer
        )
        first.start()
        second.start()
        started += [first, second]
    metas_ref[level] = meta_ref[level]
    slots = plane * capacity
    group_rows = rows_ref.shape[1]
    locals_ = []
    for d in level_order(groups):
        source = lax.rem(level + groups - d, groups)
        if d == 0:
            rows, info = rows_ref[level], meta_ref[level]
        else:
            peer = (source * plane + place, core)
            remote(meta_ref.at[source], metas_ref.at[source], m_send.at[d], m_recv.at[source], peer).wait_recv()
            remote(rows_ref.at[source], landed.at[source], z_send.at[d], z_recv.at[source], peer).wait_recv()
            rows, info = landed[source], metas_ref[source]
        info = info[:, :group_rows].astype(jnp.float32)
        slot = lax.broadcasted_iota(jnp.int32, (slots, group_rows), 0).astype(jnp.float32)
        chooser = jnp.where((slot == info[0:1]) | (slot == info[1:2]), 1.0, 0.0)
        picked = jnp.dot(chooser.astype(jnp.bfloat16), rows, preferred_element_type=jnp.float32)
        for e in range(plane):
            spread[d, e] = picked[e * capacity : (e + 1) * capacity].astype(jnp.bfloat16)
        for far in range(plane - 1, 0, -1):
            to = lax.rem(place + far, plane)
            copy = remote(
                spread.at[d, to], out_ref.at[core, source, place],
                p_send.at[d * plane + far], p_recv.at[source * plane + place],
                (level * plane + to, core),
            )
            copy.start()
            started.append(copy)
        keep = pltpu.make_async_copy(
            spread.at[d, place], out_ref.at[core, source, place], own_sem.at[d]
        )
        keep.start()
        locals_.append(keep)
    for at, d in enumerate(level_order(groups)):
        source = lax.rem(level + groups - d, groups)
        for far in range(1, plane):
            origin = lax.rem(place + plane - far, plane)
            remote(
                spread.at[d, origin], out_ref.at[core, source, origin],
                p_send.at[d * plane + far], p_recv.at[source * plane + origin],
                (level * plane + origin, core),
            ).wait_recv()
        locals_[at].wait()
        copy = remote(
            out_ref.at[core, source], out_ref.at[core, source],
            t_send.at[d], t_recv.at[source], (index, 1 - core),
        )
        copy.start()
        started.append(copy)
    for d in level_order(groups):
        source = lax.rem(level + groups - d, groups)
        remote(
            out_ref.at[1 - core, source], out_ref.at[1 - core, source],
            t_send.at[d], t_recv.at[source], (index, 1 - core),
        ).wait_recv()
    for copy in started:
        copy.wait_send()


def return_kernel(
    groups, plane, capacity, part_ref, metas_ref, out_ref,
    passed, mixed, back, merged, t_send, t_recv, p_send, p_recv, own_sem, z_send, z_recv,
):
    index, core, level, place = greet(groups, plane)
    started, locals_ = [], []
    order = level_order(groups)[::-1]
    slots = plane * capacity
    group_rows = out_ref.shape[1]
    for d in order:
        goal = lax.rem(level + d, groups)
        copy = remote(
            part_ref.at[1 - core, goal], passed.at[goal], t_send.at[d], t_recv.at[goal],
            (index, 1 - core),
        )
        copy.start()
        started.append(copy)
    for d in order:
        goal = lax.rem(level + d, groups)
        remote(
            part_ref.at[core, goal], passed.at[goal], t_send.at[d], t_recv.at[goal],
            (index, 1 - core),
        ).wait_recv()
        for e in range(plane):
            mixed[d, e] = (
                part_ref[core, goal, e].astype(jnp.float32) + passed[goal, e].astype(jnp.float32)
            ).astype(jnp.bfloat16)
        for far in range(plane - 1, 0, -1):
            to = lax.rem(place + far, plane)
            copy = remote(
                mixed.at[d, to], back.at[goal, place],
                p_send.at[d * plane + far], p_recv.at[goal * plane + place],
                (level * plane + to, core),
            )
            copy.start()
            started.append(copy)
        keep = pltpu.make_async_copy(mixed.at[d, place], back.at[goal, place], own_sem.at[d])
        keep.start()
        locals_.append(keep)
    for at, d in enumerate(order):
        goal = lax.rem(level + d, groups)
        for far in range(1, plane):
            origin = lax.rem(place + plane - far, plane)
            remote(
                mixed.at[d, origin], back.at[goal, origin],
                p_send.at[d * plane + far], p_recv.at[goal * plane + origin],
                (level * plane + origin, core),
            ).wait_recv()
        locals_[at].wait()
        info = metas_ref[goal][:, :group_rows].astype(jnp.float32)
        slot = lax.broadcasted_iota(jnp.int32, (slots, group_rows), 0).astype(jnp.float32)
        hit_first, hit_second = slot == info[0:1], slot == info[1:2]
        arrived = back[goal].reshape(slots, back.shape[-1])
        result = 0.0
        for term in range(2):
            share = jnp.where(hit_first, info[2 + term : 3 + term], 0.0) + jnp.where(
                hit_second, info[4 + term : 5 + term], 0.0
            )
            result = result + lax.dot_general(
                share.astype(jnp.bfloat16), arrived, (((0,), (0,)), ((), ())),
                preferred_element_type=jnp.float32,
            )
        if d == 0:
            out_ref[level] = result.astype(jnp.bfloat16)
        else:
            merged[d] = result.astype(jnp.bfloat16)
            copy = remote(
                merged.at[d], out_ref.at[level], z_send.at[d], z_recv.at[level],
                (goal * plane + place, core),
            )
            copy.start()
            started.append(copy)
    for d in range(1, groups):
        other = lax.rem(level + groups - d, groups)
        remote(
            merged.at[d], out_ref.at[other], z_send.at[d], z_recv.at[other],
            (other * plane + place, core),
        ).wait_recv()
    for copy in started:
        copy.wait_send()


def dispatch(rows, meta, plane, capacity):
    groups, group_rows, width = rows.shape
    vmem = pl.BlockSpec(memory_space=pltpu.VMEM)
    dma = pltpu.SemaphoreType.DMA
    few, many = dma((groups,)), dma((groups * plane,))
    return pl.pallas_call(
        functools.partial(dispatch_kernel, groups, plane, capacity),
        out_shape=(
            jax.ShapeDtypeStruct((2, groups, plane, capacity, width), jnp.bfloat16),
            jax.ShapeDtypeStruct(meta.shape, jnp.bfloat16),
        ),
        in_specs=[vmem, vmem],
        out_specs=(vmem, vmem),
        scratch_shapes=[
            pltpu.VMEM((groups, group_rows, width), jnp.bfloat16),
            pltpu.VMEM((groups, plane, capacity, width), jnp.bfloat16),
            few, few, few, few, many, many, few, few, few,
        ],
        compiler_params=pltpu.CompilerParams(
            collective_id=1, has_side_effects=True, vmem_limit_bytes=40 * 1024 * 1024
        ),
        name="dispatch",
    )(rows, meta)


def give_back(partial_value, metas, group_rows):
    _, groups, plane, capacity, width = partial_value.shape
    vmem = pl.BlockSpec(memory_space=pltpu.VMEM)
    dma = pltpu.SemaphoreType.DMA
    few, many = dma((groups,)), dma((groups * plane,))
    block = pltpu.VMEM((groups, plane, capacity, width), jnp.bfloat16)
    return pl.pallas_call(
        functools.partial(return_kernel, groups, plane, capacity),
        out_shape=jax.ShapeDtypeStruct((groups, group_rows, width), jnp.bfloat16),
        in_specs=[vmem, vmem],
        out_specs=vmem,
        scratch_shapes=[
            block, block, block,
            pltpu.VMEM((groups, group_rows, width), jnp.bfloat16),
            few, few, many, many, few, few, few,
        ],
        compiler_params=pltpu.CompilerParams(
            collective_id=2, has_side_effects=True, vmem_limit_bytes=40 * 1024 * 1024
        ),
        name="give_back",
    )(partial_value, metas)


def spread_kernel(
    groups, plane, own_ref, out_ref, z_send, z_recv, p_send, p_recv, t_send, t_recv
):
    index, core, level, place = greet(groups, plane)
    reach = groups // 2
    rows = own_ref.shape[0]
    half = rows // 2
    mine = pl.ds(pl.multiple_of(core * half, half), half)
    other = pl.ds(pl.multiple_of((1 - core) * half, half), half)

    def z_copy(d):
        return remote(
            own_ref.at[mine], out_ref.at[index, mine], z_send.at[d], z_recv.at[d],
            (lax.rem(level + d, groups) * plane + place, core),
        )

    def z_arrival(d):
        block = lax.rem(level + groups - d, groups) * plane + place
        return remote(
            own_ref.at[mine], out_ref.at[block, mine], z_send.at[d], z_recv.at[d],
            (block, core),
        )

    def p_copy(d, far):
        block = lax.rem(level + groups - d, groups) * plane + place
        source = own_ref.at[mine] if d == 0 else out_ref.at[block, mine]
        return remote(
            source, out_ref.at[block, mine], p_send.at[d * plane + far],
            p_recv.at[d * plane + far],
            (level * plane + lax.rem(place + far, plane), core),
        )

    def p_arrival(d, far):
        origin = lax.rem(place + plane - far, plane)
        block = lax.rem(level + groups - d, groups) * plane + origin
        return remote(
            own_ref.at[mine], out_ref.at[block, mine], p_send.at[d * plane + far],
            p_recv.at[d * plane + far], (level * plane + origin, core),
        )

    def t_copy(d, far, part):
        origin = lax.rem(place + plane - far, plane)
        block = lax.rem(level + groups - d, groups) * plane + origin
        return remote(
            out_ref.at[block, part], out_ref.at[block, part], t_send.at[d * plane + far],
            t_recv.at[d * plane + far], (index, 1 - core),
        )

    def wanted(d, far, sender):
        ahead = lax.rem(place + far, plane) > place if sender else place >= far
        live = level >= d
        if d == 0:
            return live & ahead
        if d == reach:
            return live & jnp.logical_not(ahead)
        return live

    for d in range(reach, 0, -1):
        pl.when(level + d < groups)(lambda d=d: z_copy(d).start())
    for far in range(1, plane):
        pl.when(wanted(0, far, True))(lambda far=far: p_copy(0, far).start())
    out_ref[index] = own_ref[...]
    for d in range(1, reach + 1):

        def arrived(d=d):
            z_arrival(d).wait_recv()
            t_copy(d, 0, mine).start()

        pl.when(level >= d)(arrived)
        for far in range(1, plane):
            pl.when(wanted(d, far, True))(lambda d=d, far=far: p_copy(d, far).start())
    for d in range(reach + 1):
        for far in range(1, plane):

            def passed_on(d=d, far=far):
                p_arrival(d, far).wait_recv()
                t_copy(d, far, mine).start()

            pl.when(wanted(d, far, False))(passed_on)
    for d in range(reach + 1):
        for far in range(0 if d else 1, plane):

            def from_partner(d=d, far=far):
                t_copy(d, far, other).wait_recv()
                t_copy(d, far, mine).wait_send()

            pl.when((level >= d) if far == 0 else wanted(d, far, False))(from_partner)
            if far:
                pl.when(wanted(d, far, True))(lambda d=d, far=far: p_copy(d, far).wait_send())
    for d in range(1, reach + 1):
        pl.when(level + d < groups)(lambda d=d: z_copy(d).wait_send())


def spread_blocks(own, count):
    rows, lanes = own.shape
    plane = count // GROUPS
    vmem = pl.BlockSpec(memory_space=pltpu.VMEM)
    few = pltpu.SemaphoreType.DMA((GROUPS,))
    many = pltpu.SemaphoreType.DMA((GROUPS * plane,))
    return pl.pallas_call(
        functools.partial(spread_kernel, GROUPS, plane),
        out_shape=jax.ShapeDtypeStruct((count, rows, lanes), jnp.bfloat16),
        in_specs=[vmem],
        out_specs=vmem,
        scratch_shapes=[few, few, many, many, many, many],
        compiler_params=pltpu.CompilerParams(
            collective_id=3, has_side_effects=True, vmem_limit_bytes=40 * 1024 * 1024
        ),
        name="spread_blocks",
    )(own).reshape(count * rows, lanes)


def local(
    residual,
    queries,
    latent,
    rope_key,
    doc_ids,
    latent_to_key,
    latent_to_value,
    out_proj,
    mix_gain,
    moe_gain,
    expert_ids,
    route_weight,
    gate_weight,
    up_weight,
    down_weight,
):
    local_rows = queries.shape[0]
    positions = lax.axis_index("sp") * local_rows + jnp.arange(local_rows, dtype=jnp.int32)
    cosine, sine = angles_of(positions)
    half = ROPE // 2
    after = HEAD_LANES - UNROTATED_DIM - ROPE
    key = rope_key.astype(jnp.float32)
    crossed = jnp.concatenate([-key[:, half:], key[:, :half]], axis=1)
    around = ((0, 0), (UNROTATED_DIM, after))
    extra = jnp.pad(key, around) * cosine + jnp.pad(crossed, around) * sine
    lane = jnp.arange(HEAD_LANES)[None, :]
    extra = jnp.where(
        lane == UNROTATED_DIM + ROPE, doc_ids.astype(jnp.float32)[:, None], extra
    ).astype(jnp.bfloat16)
    own = jnp.concatenate([latent, extra], axis=1)
    packed = spread_blocks(own, lax.axis_size("sp"))
    attended = attend(
        queries, packed, doc_ids, latent_to_key, latent_to_value, positions, cosine, sine
    )
    gathered = lax.all_to_all(attended, "tp", split_axis=0, concat_axis=1, tiled=True)
    mix = jnp.dot(gathered, out_proj, preferred_element_type=jnp.float32)
    branch = rms_scale(mix, mix_gain)
    middle = lax.optimization_barrier((residual.astype(jnp.float32) + branch).astype(jnp.bfloat16))
    normed = rms_scale(middle.astype(jnp.float32), moe_gain).astype(jnp.bfloat16)
    row_count = normed.shape[0]
    width = normed.shape[1]
    top_count = expert_ids.shape[1]
    expert_count = lax.axis_size("sp")
    capacity = row_count // (expert_count // GROUPS)
    plane = expert_count // GROUPS
    group_rows = capacity * plane // top_count
    group_of = expert_ids[:, 0] // plane
    bins = jnp.arange(expert_count + GROUPS, dtype=jnp.int32)[None, :]
    group_bin = group_of[:, None] + expert_count
    named = jnp.any(expert_ids[:, :, None] == bins[None], axis=1) | (group_bin == bins)
    before = jnp.arange(row_count)[:, None] > jnp.arange(row_count)[None, :]
    earlier = jnp.dot(
        before.astype(jnp.bfloat16), named.astype(jnp.bfloat16), preferred_element_type=jnp.float32
    ).astype(jnp.int32)
    slot_rank = jnp.sum(jnp.where(expert_ids[:, :, None] == bins[None], earlier[:, None], 0), axis=2)
    group_rank = jnp.sum(jnp.where(group_bin == bins, earlier, 0), axis=1)
    slots = lax.rem(expert_ids, plane) * capacity + slot_rank
    member = (group_of * group_rows + group_rank)[:, None]
    chooser = (member == jnp.arange(GROUPS * group_rows, dtype=jnp.int32)[None, :]).astype(
        jnp.bfloat16
    )
    coarse = route_weight.astype(jnp.bfloat16)
    fine = (route_weight - coarse.astype(jnp.float32)).astype(jnp.bfloat16)
    fields = jnp.concatenate(
        [
            (slots + 1).astype(jnp.bfloat16),
            jnp.stack([coarse[:, 0], fine[:, 0], coarse[:, 1], fine[:, 1]], axis=1),
        ],
        axis=1,
    )
    fields = jnp.pad(fields, ((0, 0), (0, 16 - fields.shape[1])))
    meta = lax.dot_general(
        fields, chooser, (((0,), (0,)), ((), ())), preferred_element_type=jnp.float32
    )
    meta = meta - (jnp.arange(16) < top_count)[:, None].astype(jnp.float32)
    meta = meta.astype(jnp.bfloat16).reshape(16, GROUPS, group_rows).transpose(1, 0, 2)
    meta = jnp.pad(meta, ((0, 0), (0, 0), (0, -group_rows % 128)))
    grouped = lax.dot_general(
        chooser, normed, (((0,), (0,)), ((), ())), preferred_element_type=jnp.float32
    ).astype(jnp.bfloat16)
    arrived, metas = dispatch(
        grouped.reshape(GROUPS, group_rows, width), meta, plane, capacity
    )
    flat_rows = arrived.reshape(-1, width)
    gate_out = jnp.dot(flat_rows, gate_weight[0], preferred_element_type=jnp.float32)
    upward = jnp.dot(flat_rows, up_weight[0], preferred_element_type=jnp.float32)
    hidden = (jax.nn.silu(gate_out) * upward).astype(jnp.bfloat16)
    partial_value = jnp.dot(hidden, down_weight[0], preferred_element_type=jnp.float32)
    returned = give_back(
        partial_value.astype(jnp.bfloat16).reshape(arrived.shape), metas, group_rows
    )
    expert_mix = jnp.dot(
        chooser, returned.reshape(-1, width), preferred_element_type=jnp.float32
    )
    return (middle.astype(jnp.float32) + expert_mix).astype(jnp.bfloat16)


def solution(mesh):
    in_specs = (
        P(("sp", "tp"), None),
        P("sp", "tp"),
        P("sp", None),
        P("sp", None),
        P("sp"),
        P(None, "tp"),
        P(None, "tp"),
        P(),
        P(),
        P(),
        P(("sp", "tp"), None),
        P(("sp", "tp"), None),
        P("sp", None, "tp"),
        P("sp", None, "tp"),
        P("sp", "tp", None),
    )
    out_specs = P(("sp", "tp"), None)
    return jax.shard_map(local, mesh=mesh, in_specs=in_specs, out_specs=out_specs, check_vma=False)
```
